256 devices in a mesh: kv: 64 (over z, x, core), tp: 4 (over y).
Axes of the slice: x: 4, y: 4, z: 8, core: 2. Of those that a mesh axis runs over, the one named last changes fastest.
Arguments:
- normed_input: bfloat16 [32768, 4096], P('kv', 'tp'), may hold values from -0.13183594 to 0.13183594
- queries: bfloat16 [32768, 2048], P('kv', 'tp'), may hold values from -1.5 to 1.5
- key_rows: bfloat16 [32768, 2048], P('kv', 'tp'), may hold values from -1.5 to 1.5
- value_rows: bfloat16 [32768, 2048], P('kv', 'tp'), may hold values from -6 to 6
- log_sums: float32 [32, 32768], P('tp', 'kv'), may hold values from -0.5 to 10
- cotangent: bfloat16 [32768, 2048], P('kv', 'tp'), may hold values from -48 to 48
- block_list: int32 [64, 16], P('kv'), may hold values from -1 to 1023, as said below
Outputs:
- grad_queries: float32 [32768, 2048], P('kv', 'tp')
- grad_keys: float32 [32768, 2048], P('kv', 'tp')
- grad_values: float32 [32768, 2048], P('kv', 'tp')
- grad_weight: float32 [4096, 2048], P('kv', 'tp')
The draws below stay inside these ranges and needn't reach their ends.
Inputs may be any that keep to these rules, and one draw needn't show every extreme that they name: `block_list`: row d names the key blocks chosen by query block d: distinct blocks that all lie on devices of kv index below d (block g on index g // 16), at most 1 of them on one index, named entries first and -1 after them; row d has between min(8, d) and min(16, d) named entries, and the last row has 16 and names a block on index 0.
All inputs are finite; a program needn't handle non-finite values.
Results may differ from the reference program's by a relative error of at most 0.0041.
Values may be sent and summed in bfloat16 or wider, within the bound.
A program may use at most 128 MiB of HBM per device.

```python
import jax
import jax.numpy as jnp
from jax import lax

D = 4096
HEADS = 32
HD = 64
KB = 32
MOST = 16
TOK_DEV = 512
TOKENS = 32768
N_KV = 64


def chosen_blocks(base_key):
    block_count = TOK_DEV // KB
    capacity = max(1, 2 * MOST // N_KV)
    streams = jax.random.split(jax.random.fold_in(base_key, 17), 3)
    devices = jnp.arange(N_KV)
    raw_order = jax.random.randint(streams[0], (N_KV, N_KV, block_count), 0, 1 << 16)
    locals_drawn = jnp.argsort(raw_order * block_count + jnp.arange(block_count), axis=-1, stable=True)[..., :capacity]
    drawn_prio = jax.random.randint(streams[1], (N_KV, N_KV, capacity), 0, 1 << 12)
    owner_dev = jnp.arange(N_KV)[None, :, None]
    member = jnp.arange(capacity)[None, None, :]
    source = devices[:, None, None]
    item_id = owner_dev * capacity + member
    priority = drawn_prio * (N_KV * capacity) + item_id
    priority = priority + jnp.where(owner_dev == source - 1, 1 << 26, 0)
    priority = priority + jnp.where((owner_dev == source - N_KV // 2) & (member == 0), 1 << 25, 0)
    priority = priority + jnp.where((owner_dev == 0) & (source == N_KV - 1) & (member == 0), 1 << 24, 0)
    priority = jnp.where(owner_dev < source, priority, -1 - item_id)
    top_prio, top_item = lax.top_k(priority.reshape(N_KV, N_KV * capacity), MOST)
    owners_sel = top_item // capacity
    blocks_sel = jnp.take_along_axis(locals_drawn.reshape(N_KV, N_KV * capacity), top_item, axis=1)
    halfway = MOST // 2
    drawn_count = jax.random.randint(streams[2], (N_KV,), 0, halfway + 1)
    counts = halfway + drawn_count * drawn_count // max(halfway, 1)
    counts = counts.at[N_KV - 1].set(MOST)
    counts = jnp.minimum(counts, devices * capacity)
    active = jnp.arange(MOST)[None, :] < counts[:, None]
    return jnp.where(active, owners_sel * block_count + blocks_sel, -1).astype(jnp.int32)


def draw_block_list(key, part):
    return chosen_blocks(key)


def draw_log_sums(key, part):
    listed = chosen_blocks(key)
    counts = jnp.sum((listed >= 0).astype(jnp.int32), axis=1)
    position = jnp.arange(TOKENS)
    seen = position % TOK_DEV + 1 + KB * counts[position // TOK_DEV]
    base = jnp.log(seen.astype(jnp.float32))
    noise_key = jax.random.fold_in(key, 29)
    jitter = jax.random.uniform(noise_key, (HEADS, TOKENS), jnp.float32, -0.25, 0.75)
    return base[None, :] + jitter


def shard_levels(key, extent, cuts, low, largest):
    loudness = 1.0
    for dim, parts in cuts:
        steps = jax.random.uniform(jax.random.fold_in(jax.random.fold_in(key, 6), dim), (parts,), jnp.float32, low / len(cuts), largest / len(cuts))
        loudness = loudness * jnp.repeat(jnp.exp(steps), extent[dim] // parts).reshape((-1,) + (1,) * (len(extent) - 1 - dim))
    return loudness


def scatter_about(rng, extent, deviation, bound, cuts=(), kind=jnp.bfloat16):
    values = jax.random.normal(rng, extent, jnp.float32) * deviation
    if len(cuts) > 0:
        values = shard_levels(rng, extent, cuts, -0.22, 0.18) * values
    return jnp.clip(values, min=-bound, max=bound).astype(kind)


def setup_inputs(seed: int = 0) -> dict:
    keys = jax.random.split(jax.random.key(seed), 8)
    return {
        "normed_input": scatter_about(keys[0], (TOKENS, D), (4.0 * TOKENS ** -0.5), 0.13183594, ((0, 64), (1, 4))),
        "queries": jnp.clip(jax.random.uniform(keys[1], (TOKENS, HEADS * HD), jnp.float32, -1.5, 1.5) * shard_levels(keys[1], (TOKENS, HEADS * HD), ((0, 64), (1, 4)), -0.4, 0.0), -1.5, 1.5).astype(jnp.bfloat16),
        "key_rows": jnp.clip(jax.random.uniform(keys[2], (TOKENS, HEADS * HD), jnp.float32, -1.5, 1.5) * shard_levels(keys[2], (TOKENS, HEADS * HD), ((0, 64), (1, 4)), -0.4, 0.0), -1.5, 1.5).astype(jnp.bfloat16),
        "value_rows": scatter_about(keys[3], (TOKENS, HEADS * HD), 1.0, 6.0, ((0, 64), (1, 4))),
        "log_sums": draw_log_sums(jax.random.fold_in(keys[7], 71), 0),
        "cotangent": scatter_about(keys[5], (TOKENS, HEADS * HD), 8.0, 48.0, ((0, 64), (1, 4))),
        "block_list": draw_block_list(jax.random.fold_in(keys[7], 71), 0),
    }


def contract(former, latter, former_dim, latter_dim):
    return lax.dot_general(former, latter, (((former_dim,), (latter_dim,)), ((), ())), preferred_element_type=jnp.float32)


def head_terms(query_part, keys_own, values_own, keys_sel, values_sel, grad_out, log_sum, own_mask, sel_mask):
    scaling = HD ** -0.5

    def forward(key_part, value_part, mask_part):
        scores = contract(query_part, key_part, 1, 1) * scaling
        probability = jnp.where(mask_part, jnp.exp(scores - log_sum[:, None]), 0.0)
        pulled = contract(grad_out, value_part, 1, 1)
        return probability, pulled

    prob_own, pull_own = forward(keys_own, values_own, own_mask)
    prob_sel, pull_sel = forward(keys_sel, values_sel, sel_mask)
    row_dot = jnp.sum(prob_own * pull_own, axis=1) + jnp.sum(prob_sel * pull_sel, axis=1)

    def backward(prob_part, pull_part, key_part):
        dscore = (prob_part * (pull_part - row_dot[:, None])).astype(jnp.bfloat16)
        rounded = prob_part.astype(jnp.bfloat16)
        return (contract(dscore, key_part, 1, 0), scaling * contract(dscore, query_part, 0, 0), contract(rounded, grad_out, 0, 0))

    own_terms = backward(prob_own, pull_own, keys_own)
    sel_terms = backward(prob_sel, pull_sel, keys_sel)
    return (scaling * (own_terms[0] + sel_terms[0]), own_terms[1], own_terms[2], sel_terms[1], sel_terms[2])


def reference(normed_input, queries, key_rows, value_rows, log_sums, cotangent, block_list):
    width_all = queries.shape[1]
    head_count = width_all // HD

    def heads_first(array):
        return array.reshape(array.shape[0], head_count, HD).transpose(1, 0, 2)

    query_heads = heads_first(queries)
    key_heads = heads_first(key_rows)
    value_heads = heads_first(value_rows)
    grad_heads = heads_first(cotangent)
    position = jnp.arange(TOK_DEV, dtype=jnp.int32)
    own_mask = position[:, None] >= position[None, :]
    key_span = jnp.arange(KB, dtype=jnp.int32)

    def step(carry, device):
        key_grad, value_grad = carry
        offset = (device * TOK_DEV).astype(jnp.int32)

        def own_slice(array):
            return lax.dynamic_slice_in_dim(array, offset, TOK_DEV, 1)

        listed = block_list[device]
        active = listed >= 0
        sel_rows = (jnp.where(active, listed, 0)[:, None] * KB + key_span[None, :]).reshape(-1).astype(jnp.int32)
        sel_mask = jnp.broadcast_to(jnp.repeat(active, KB)[None, :], (TOK_DEV, MOST * KB))

        def per_head(pieces):
            query_part, keys_own, values_own, grad_out, log_sum, keys_all, values_all = pieces
            return head_terms(query_part, keys_own, values_own, keys_all[sel_rows], values_all[sel_rows], grad_out, log_sum, own_mask, sel_mask)

        results = lax.map(per_head, (own_slice(query_heads), own_slice(key_heads), own_slice(value_heads), own_slice(grad_heads), own_slice(log_sums), key_heads, value_heads))
        sel_keys = results[3].astype(jnp.bfloat16).astype(jnp.float32)
        sel_values = results[4].astype(jnp.bfloat16).astype(jnp.float32)
        own_rows = offset + position
        key_grad = key_grad.at[:, own_rows].add(results[1]).at[:, sel_rows].add(sel_keys)
        value_grad = value_grad.at[:, own_rows].add(results[2]).at[:, sel_rows].add(sel_values)
        return (key_grad, value_grad), results[0]

    empty_grad = jnp.zeros((head_count, TOK_DEV * N_KV, HD), jnp.float32)
    (key_grad, value_grad), query_grad = lax.scan(step, (empty_grad, empty_grad), jnp.arange(N_KV, dtype=jnp.int32))
    grad_queries = query_grad.transpose(0, 2, 1, 3).reshape(TOK_DEV * N_KV, width_all)
    grad_keys = key_grad.transpose(1, 0, 2).reshape(TOK_DEV * N_KV, width_all)
    grad_values = value_grad.transpose(1, 0, 2).reshape(TOK_DEV * N_KV, width_all)
    query_b = grad_queries.astype(jnp.bfloat16)
    grad_weight = jnp.dot(normed_input.T, query_b, preferred_element_type=jnp.float32)
    return grad_queries, grad_keys, grad_values, grad_weight
```

```python
import functools

import jax
import jax.numpy as jnp
from jax import lax
from jax.experimental import pallas as pl
from jax.experimental.pallas import tpu as pltpu
from jax.sharding import PartitionSpec as P

MESH = pl.DeviceIdType.MESH
HD = 64
KB = 32
MOST = 16
TOK = 512
NZ = 8
NG = 8
NY = 4
NX = 4
SLOTS = NZ * (NZ + 1) // 2
BPD = TOK // KB
F32 = jnp.float32
BF16 = jnp.bfloat16
Z_ORDER = (4, 3, 5, 2, 6, 1, 7)
G_ORDER = (4, 5, 3, 2, 6, 7, 1)


def here():
    kv = lax.axis_index("kv")
    return kv, lax.div(kv, NG), lax.rem(kv, NG), lax.axis_index("tp")


def remote(src, dst, send_sem, recv_sem, target):
    return pltpu.make_async_remote_copy(
        src_ref=src, dst_ref=dst, send_sem=send_sem, recv_sem=recv_sem, device_id=target, device_id_type=MESH
    )


def signal(sem, target):
    pl.semaphore_signal(sem, inc=1, device_id=target, device_id_type=MESH)


def gather_kernel(
    q_ref, k_ref, v_ref, o_ref, lse_ref, list_ref, a_ref,
    kvr_ref, qor_ref, lser_ref, xr_ref, ag_ref, t_ref, w_ref,
    kvp, qop, lsp, tb, xs, wsm,
    kv_s, kv_r, qo_s, qo_r, ls_s, ls_r, tb_s, tb_r, xs_s, xs_r, a_s, a_r, loc,
):
    kv, z, g, y = here()
    right, left = lax.rem(y + 1, NY), lax.rem(y + NY - 1, NY)
    planes = NZ * NG

    bar = pltpu.get_barrier_semaphore()

    def greet(i, c):
        signal(bar, {"kv": lax.rem(kv + i, planes)})
        return c

    lax.fori_loop(1, planes, greet, 0)
    signal(bar, {"tp": right})
    signal(bar, {"tp": left})

    rows = 64
    low = lax.broadcasted_iota(jnp.int32, (rows, 128), 1) < HD

    def pack(i, c):
        r = pl.ds(pl.multiple_of(i * rows, rows), rows)
        for first, second, out in ((k_ref, v_ref, kvp), (q_ref, o_ref, qop)):
            for p in range(4):
                a = first[r, 128 * p : 128 * p + 128].astype(F32)
                b = second[r, 128 * p : 128 * p + 128].astype(F32)
                first_head = jnp.where(low, a, pltpu.roll(b, HD, 1)).astype(BF16)
                second_head = jnp.where(low, pltpu.roll(a, HD, 1), b).astype(BF16)
                for j in range(rows // KB):
                    at = i * (rows // KB) + j
                    out[2 * p, at] = first_head[KB * j : KB * j + KB]
                    out[2 * p + 1, at] = second_head[KB * j : KB * j + KB]
        return c

    lax.fori_loop(0, TOK // rows, pack, 0)
    for h in range(NZ):
        lsp[h] = lse_ref[h : h + 1, :]
    tb[kv] = list_ref[...]
    kvr_ref[z] = kvp[z]

    pl.semaphore_wait(bar, planes - 1 + 2)

    def table_copy(peer, slot):
        return remote(tb.at[slot], tb.at[slot], tb_s.at[peer], tb_r.at[slot], {"kv": peer})

    def send_table(i, c):
        table_copy(lax.rem(kv + i, planes), kv).start()
        return c

    lax.fori_loop(1, planes, send_table, 0)

    to_right = remote(a_ref, ag_ref.at[0], a_s.at[0], a_r.at[0], {"tp": right})
    to_left = remote(a_ref, ag_ref.at[1], a_s.at[1], a_r.at[1], {"tp": left})
    to_right.start()
    to_left.start()

    def kv_copy(zt, slot):
        return remote(kvp.at[zt], kvr_ref.at[slot], kv_s.at[zt], kv_r.at[slot], {"kv": zt * NG + g})

    def qo_copy(zt, slot):
        return remote(qop.at[zt], qor_ref.at[slot], qo_s.at[zt], qo_r.at[slot], {"kv": zt * NG + g})

    def ls_copy(zt, slot):
        return remote(lsp.at[zt], lser_ref.at[slot], ls_s.at[zt], ls_r.at[slot], {"kv": zt * NG + g})

    for off in Z_ORDER:
        kv_copy(lax.rem(z + off, NZ), z).start()
    for off in Z_ORDER:
        zt = lax.rem(z + off, NZ)
        qo_copy(zt, z).start()
        ls_copy(zt, z).start()
    own_qo = pltpu.make_async_copy(qop.at[z], qor_ref.at[z], loc.at[0])
    own_ls = pltpu.make_async_copy(lsp.at[z], lser_ref.at[z], loc.at[1])
    own_qo.start()
    own_ls.start()

    def wait_table(i, c):
        peer = lax.rem(kv + i, planes)
        table_copy(peer, peer).wait_recv()
        return c

    lax.fori_loop(1, planes, wait_table, 0)

    table = tb[:, 0, :]
    t_ref[...] = table
    lanes = lax.broadcasted_iota(jnp.int32, (planes, 128), 1)
    want = jnp.full((planes, 128), -1, jnp.int32)
    for s in range(MOST):
        col = table[:, s : s + 1]
        want = jnp.where(lax.shift_right_arithmetic(col, 4) == lanes, jnp.bitwise_and(col, BPD - 1), want)
    w_ref[...] = want
    to_smem = pltpu.make_async_copy(w_ref, wsm, loc.at[2])
    to_smem.start()
    to_smem.wait()

    for off in Z_ORDER:
        zs = lax.rem(z + NZ - off, NZ)
        kv_copy(zs, zs).wait_recv()

    def x_copy(gp, slot):
        return remote(xs.at[gp], xr_ref.at[slot], xs_s.at[gp], xs_r.at[slot], {"kv": z * NG + gp})

    def choose(gp):
        for zd in range(NZ):
            for zo in range(zd + 1):
                b = jnp.maximum(wsm[zd * NG + gp, zo * NG + g], 0)
                xs[gp, zd * (zd + 1) // 2 + zo] = kvr_ref[zo, b]

    def pick(i, c):
        gp = lax.rem(g + i, NG)
        choose(gp)
        x_copy(gp, g).start()
        return c

    lax.fori_loop(1, NG, pick, 0)
    choose(g)
    own_x = pltpu.make_async_copy(xs.at[g], xr_ref.at[g], loc.at[3])
    own_x.start()

    half = TOK // 2
    on_right = remote(
        ag_ref.at[0, pl.ds(0, half)], ag_ref.at[2, pl.ds(0, half)], a_s.at[2], a_r.at[2], {"tp": right}
    )
    on_left = remote(
        ag_ref.at[1, pl.ds(half, half)], ag_ref.at[2, pl.ds(half, half)], a_s.at[3], a_r.at[3], {"tp": left}
    )
    to_right.wait_recv()
    on_right.start()
    to_left.wait_recv()
    on_left.start()

    for off in Z_ORDER:
        zs = lax.rem(z + NZ - off, NZ)
        qo_copy(zs, zs).wait_recv()
        ls_copy(zs, zs).wait_recv()

    def wait_x(i, c):
        gp = lax.rem(g + i, NG)
        x_copy(gp, gp).wait_recv()
        x_copy(gp, g).wait_send()
        return c

    lax.fori_loop(1, NG, wait_x, 0)

    def drain_table(i, c):
        table_copy(lax.rem(kv + i, planes), kv).wait_send()
        return c

    lax.fori_loop(1, planes, drain_table, 0)
    for off in Z_ORDER:
        zt = lax.rem(z + off, NZ)
        kv_copy(zt, z).wait_send()
        qo_copy(zt, z).wait_send()
        ls_copy(zt, z).wait_send()
    to_right.wait_send()
    to_left.wait_send()
    on_right.wait()
    on_left.wait()
    own_qo.wait()
    own_ls.wait()
    own_x.wait()


def attention_kernel(t_ref, qo_ref, kv_ref, lse_ref, xr_ref, dq_ref, dkvo_ref, rb_ref, sel, qs, om, p_scr, u_scr, rd, dq):
    zd = pl.program_id(0)
    g = lax.rem(lax.axis_index("kv"), NG)
    d = zd * NG + g
    base = lax.div(zd * (zd + 1), 2)

    @pl.when(zd == 0)
    def _():
        rb_ref[...] = jnp.zeros_like(rb_ref)

    count = jnp.int32(0)
    for s in range(MOST):
        entry = t_ref[d, s]
        count = count + jnp.where(entry >= 0, 1, 0)
        owner = lax.shift_right_arithmetic(jnp.maximum(entry, 0), 4)
        sel[KB * s : KB * s + KB, :] = xr_ref[jnp.bitwise_and(owner, NG - 1), base + lax.shift_right_arithmetic(owner, 3)]

    low = lax.broadcasted_iota(jnp.int32, (TOK, 128), 1) < HD
    both = qo_ref[0].reshape(TOK, 128).astype(F32)
    qs[...] = jnp.where(low, both * (HD ** -0.5), 0.0).astype(BF16)
    om[...] = jnp.where(low, 0.0, both).astype(BF16)
    rd[...] = jnp.zeros_like(rd)
    dq[...] = jnp.zeros_like(dq)
    half = TOK // 2
    nt = (((1,), (1,)), ((), ()))

    def forward(block, row, q0):
        st = lax.dot_general(block, qs[q0:, :], nt, preferred_element_type=F32)
        ut = lax.dot_general(block, om[q0:, :], nt, preferred_element_type=F32)
        key = lax.broadcasted_iota(jnp.int32, st.shape, 0) + (row % TOK)
        if row < TOK:
            keep = key <= lax.broadcasted_iota(jnp.int32, st.shape, 1) + q0
        else:
            keep = key < count * KB
        p = jnp.where(keep, jnp.exp(st - lse_ref[0, :, q0:]), 0.0)
        p_scr[row : row + half, q0:] = p
        u_scr[row : row + half, q0:] = ut
        rd[:, q0:] += jnp.sum(p * ut, axis=0, keepdims=True)

    def backward(block, row, q0):
        p = p_scr[row : row + half, q0:]
        ds = (p * (u_scr[row : row + half, q0:] - rd[:, q0:])).astype(BF16)
        dq[:, q0:] += jnp.dot(block.T[:HD, :], ds, preferred_element_type=F32)
        dkv = jnp.dot(ds, qs[q0:, :], preferred_element_type=F32)
        dkv += jnp.dot(p.astype(BF16), om[q0:, :], preferred_element_type=F32)
        if row < TOK:
            dkvo_ref[0, row : row + half, :] = dkv
            return
        dkv = dkv.astype(BF16)
        for i in range(half // KB):
            entry = t_ref[d, (row - TOK) // KB + i]
            owner = lax.shift_right_arithmetic(entry, 4)

            @pl.when(entry >= 0)
            def _(i=i, owner=owner):
                rb_ref[jnp.bitwise_and(owner, NG - 1), base + lax.shift_right_arithmetic(owner, 3)] = dkv[
                    KB * i : KB * i + KB
                ]

    own = kv_ref[0].reshape(TOK, 128)
    forward(own[:half], 0, 0)
    forward(own[half:], half, half)
    forward(sel[:half, :], TOK, 0)
    pl.when(count > MOST // 2)(lambda: forward(sel[half:, :], TOK + half, 0))
    backward(own[:half], 0, 0)
    backward(own[half:], half, half)
    backward(sel[:half, :], TOK, 0)
    pl.when(count > MOST // 2)(lambda: backward(sel[half:, :], TOK + half, 0))
    dq_ref[0] = (dq[...] * (HD ** -0.5)).astype(BF16)


def product_kernel(
    dq_ref, rb_ref, a_ref, ag_ref,
    qbt_ref, rbr_ref, s1_ref,
    abuf, qb, keep, cs, cr,
    dq_s, dq_r, rb_s, rb_r, c_s, c_r, loc,
):
    kv, z, g, y = here()
    core = lax.rem(kv, 2)
    partner = kv + 1 - 2 * core
    loads = [pltpu.make_async_copy(a_ref, abuf.at[0], loc.at[0])]
    loads += [pltpu.make_async_copy(ag_ref.at[j], abuf.at[j + 1], loc.at[j + 1]) for j in range(NY - 1)]
    bar = pltpu.get_barrier_semaphore()
    for i in range(1, NZ):
        signal(bar, {"kv": lax.rem(z + i, NZ) * NG + g})
        signal(bar, {"kv": z * NG + lax.rem(g + i, NG)})
    for load in loads:
        load.start()
    qbt_ref[z] = dq_ref[z]
    pl.semaphore_wait(bar, NZ - 1 + NG - 1)

    def dq_copy(zt, slot):
        return remote(dq_ref.at[zt], qbt_ref.at[slot], dq_s.at[zt], dq_r.at[slot], {"kv": zt * NG + g})

    def rb_copy(gp, slot):
        return remote(rb_ref.at[gp], rbr_ref.at[slot], rb_s.at[gp], rb_r.at[slot], {"kv": z * NG + gp})

    for off in Z_ORDER:
        dq_copy(lax.rem(z + off, NZ), z).start()
    for off in G_ORDER:
        rb_copy(lax.rem(g + off, NG), g).start()
    own_rb = pltpu.make_async_copy(rb_ref.at[g], rbr_ref.at[g], loc.at[NY])
    own_rb.start()
    for off in Z_ORDER:
        zs = lax.rem(z + NZ - off, NZ)
        dq_copy(zs, zs).wait_recv()

    for h in range(NZ):
        qb[:, HD * h : HD * h + HD] = qbt_ref[h].astype(F32).T.astype(BF16)

    def core_copy(yb):
        part = pl.ds(yb * 8, 8)
        return remote(cs.at[part], cr.at[part], c_s.at[yb], c_r.at[yb], {"kv": partner})

    owners = (y, lax.rem(y + NY - 1, NY), lax.rem(y + 1, NY), lax.rem(y + 2, NY))
    for j in range(NY):
        loads[j].wait()
        yb = owners[j]

        def strip(m, c, j=j, yb=yb):
            a = abuf[j, :, pl.ds(pl.multiple_of(m * 128, 128), 128)]
            acc = lax.dot_general(a, qb[...], (((0,), (0,)), ((), ())), preferred_element_type=F32)
            lo, hi = acc[:HD, :], acc[HD:, :]
            keep[yb * 8 + m] = jnp.where(core == 0, lo, hi)
            cs[yb * 8 + m] = jnp.where(core == 0, hi, lo).astype(BF16)
            return c

        lax.fori_loop(0, 8, strip, 0)
        core_copy(yb).start()
    for j in range(NY):
        yb = owners[j]
        core_copy(yb).wait_recv()

        def add(m, c, yb=yb):
            i = yb * 8 + m
            s1_ref[i] = (keep[i] + cr[i].astype(F32)).astype(BF16)
            return c

        lax.fori_loop(0, 8, add, 0)

    for off in G_ORDER:
        gp = lax.rem(g + off, NG)
        rb_copy(gp, gp).wait_recv()
        rb_copy(gp, g).wait_send()
    for off in Z_ORDER:
        dq_copy(lax.rem(z + off, NZ), z).wait_send()
    for j in range(NY):
        core_copy(owners[j]).wait_send()
    own_rb.wait()


def collect_kernel(w_ref, own_ref, rbr_ref, out_ref, acc):
    zo = pl.program_id(0)
    o = zo * NG + lax.rem(lax.axis_index("kv"), NG)
    acc[...] = own_ref[0]

    def add(zd, c):
        for gd in range(NG):
            b = w_ref[zd * NG + gd, o]

            @pl.when(b >= 0)
            def _(b=b, gd=gd):
                at = pl.ds(pl.multiple_of(b * KB, KB), KB)
                acc[at, :] += rbr_ref[gd, lax.div(zd * (zd + 1), 2) + zo].astype(F32)

        return c

    lax.fori_loop(zo, NZ, add, 0)
    out_ref[0] = acc[...].astype(BF16)


def return_kernel(
    dkv_ref, s1_ref,
    dkvr_ref, gw_ref,
    relay, fixed, last_l, last_r, s2, zr,
    dk_s, dk_r, f_s, f_r, n_s, n_r, l_s, l_r, z_s, z_r, loc,
):
    kv, z, g, y = here()
    core = lax.rem(kv, 2)
    x = lax.div(g, 2)

    def at_x(t):
        return {"kv": z * NG + lax.rem(t, NX) * 2 + core}

    right, left, far = x + 1, x + NX - 1, lax.rem(x + 2, NX)
    bar = pltpu.get_barrier_semaphore()
    for i in range(1, NZ):
        signal(bar, {"kv": lax.rem(z + i, NZ) * NG + g})
    signal(bar, at_x(right))
    signal(bar, at_x(left))
    pl.semaphore_wait(bar, NZ - 1 + 2)

    def piece(zz, t):
        return zz * NX + lax.rem(t, NX)

    def first(zz):
        ahead = right if zz % 2 == 0 else left
        return remote(s1_ref.at[piece(zz, far)], relay.at[zz], f_s.at[zz], f_r.at[zz], at_x(ahead))

    def direct(zz):
        back = left if zz % 2 == 0 else right
        into = last_r if zz % 2 == 0 else last_l
        return remote(s1_ref.at[piece(zz, back)], into.at[zz], n_s.at[zz], n_r.at[zz], at_x(back))

    def summed(zz):
        ahead = right if zz % 2 == 0 else left
        into = last_l if zz % 2 == 0 else last_r
        return remote(fixed.at[zz], into.at[zz], l_s.at[zz], l_r.at[zz], at_x(ahead))

    def dkv_copy(zt, slot):
        return remote(dkv_ref.at[zt], dkvr_ref.at[slot], dk_s.at[zt], dk_r.at[slot], {"kv": zt * NG + g})

    for zz in range(NZ):
        first(zz).start()
    for zz in range(NZ):
        direct(zz).start()
    for off in Z_ORDER:
        dkv_copy(lax.rem(z + off, NZ), z).start()
    own = pltpu.make_async_copy(dkv_ref.at[z], dkvr_ref.at[z], loc.at[0])
    own.start()

    for zz in range(NZ):
        ahead = right if zz % 2 == 0 else left
        first(zz).wait_recv()
        fixed[zz] = (relay[zz].astype(F32) + s1_ref[piece(zz, ahead)].astype(F32)).astype(BF16)
        summed(zz).start()

    def z_copy(zt, slot):
        return remote(s2.at[zt], zr.at[slot], z_s.at[zt], z_r.at[slot], {"kv": zt * NG + g})

    for zz in range(NZ):
        direct(zz).wait_recv()
        summed(zz).wait_recv()
        total = s1_ref[piece(zz, x)].astype(F32) + last_l[zz].astype(F32) + last_r[zz].astype(F32)
        s2[zz] = total.astype(BF16)

        @pl.when(zz != z)
        def _(zz=zz):
            z_copy(zz, z).start()

        @pl.when(zz == z)
        def _(total=total):
            gw_ref[...] = total

    for off in range(1, NZ):
        zs = lax.rem(z + off, NZ)
        z_copy(zs, zs).wait_recv()
        gw_ref[...] += zr[zs].astype(F32)

    for off in Z_ORDER:
        zs = lax.rem(z + NZ - off, NZ)
        dkv_copy(zs, zs).wait_recv()
    for zz in range(NZ):
        first(zz).wait_send()
        direct(zz).wait_send()
        summed(zz).wait_send()
    for off in Z_ORDER:
        zt = lax.rem(z + off, NZ)
        dkv_copy(zt, z).wait_send()
        z_copy(zt, z).wait_send()
    own.wait()


def unpack_kernel(qbt_ref, dkv_ref, gq_ref, gk_ref, gv_ref):
    gq_ref[...] = qbt_ref[...].astype(F32).reshape(128, TOK).T
    a = dkv_ref[0].astype(F32)
    b = dkv_ref[1].astype(F32)
    low = lax.broadcasted_iota(jnp.int32, (TOK, 128), 1) < HD
    gk_ref[...] = jnp.where(low, a, pltpu.roll(b, HD, 1))
    gv_ref[...] = jnp.where(low, pltpu.roll(a, HD, 1), b)


def per_device(normed_input, queries, key_rows, value_rows, log_sums, cotangent, block_list):
    vmem = pl.BlockSpec(memory_space=pltpu.VMEM)
    smem = pl.BlockSpec(memory_space=pltpu.SMEM)
    hbm = pl.BlockSpec(memory_space=pl.ANY)
    dma = pltpu.SemaphoreType.DMA
    shape = jax.ShapeDtypeStruct
    planes = NZ * NG
    listed = jnp.pad(block_list, ((0, 7), (0, 128 - MOST)), constant_values=-1)

    kvr, qor, lser, xr, ag, table, want = pl.pallas_call(
        gather_kernel,
        out_shape=(
            shape((NZ, BPD, KB, 128), BF16),
            shape((NZ, BPD, KB, 128), BF16),
            shape((NZ, 1, TOK), F32),
            shape((NG, SLOTS, KB, 128), BF16),
            shape((NY - 1, TOK, normed_input.shape[1]), BF16),
            shape((planes, 128), jnp.int32),
            shape((planes, 128), jnp.int32),
        ),
        in_specs=[vmem] * 6 + [hbm],
        out_specs=(vmem, hbm, hbm, hbm, hbm, vmem, vmem),
        scratch_shapes=[
            pltpu.VMEM((NZ, BPD, KB, 128), BF16),
            pltpu.VMEM((NZ, BPD, KB, 128), BF16),
            pltpu.VMEM((NZ, 1, TOK), F32),
            pltpu.VMEM((planes, 8, 128), jnp.int32),
            pltpu.VMEM((NG, SLOTS, KB, 128), BF16),
            pltpu.SMEM((planes, 128), jnp.int32),
            dma((NZ,)), dma((NZ,)), dma((NZ,)), dma((NZ,)), dma((NZ,)), dma((NZ,)),
            dma((planes,)), dma((planes,)), dma((NG,)), dma((NG,)), dma((4,)), dma((4,)), dma((4,)),
        ],
        compiler_params=pltpu.CompilerParams(collective_id=0, has_side_effects=True),
        name="gather",
    )(queries, key_rows, value_rows, cotangent, log_sums, listed, normed_input)

    dqt, dkvo, rb = pl.pallas_call(
        attention_kernel,
        grid=(NZ,),
        out_shape=(
            shape((NZ, HD, TOK), BF16),
            shape((NZ, TOK, 128), F32),
            shape((NG, SLOTS, KB, 128), BF16),
        ),
        in_specs=[
            smem,
            pl.BlockSpec((1, BPD, KB, 128), lambda i: (i, 0, 0, 0)),
            pl.BlockSpec((1, BPD, KB, 128), lambda i: (i, 0, 0, 0)),
            pl.BlockSpec((1, 1, TOK), lambda i: (i, 0, 0)),
            pl.BlockSpec((NG, SLOTS, KB, 128), lambda i: (0, 0, 0, 0)),
        ],
        out_specs=(
            pl.BlockSpec((1, HD, TOK), lambda i: (i, 0, 0)),
            pl.BlockSpec((1, TOK, 128), lambda i: (i, 0, 0)),
            pl.BlockSpec((NG, SLOTS, KB, 128), lambda i: (0, 0, 0, 0)),
        ),
        scratch_shapes=[
            pltpu.VMEM((TOK, 128), BF16),
            pltpu.VMEM((TOK, 128), BF16),
            pltpu.VMEM((TOK, 128), BF16),
            pltpu.VMEM((2 * TOK, TOK), F32),
            pltpu.VMEM((2 * TOK, TOK), F32),
            pltpu.VMEM((1, TOK), F32),
            pltpu.VMEM((HD, TOK), F32),
        ],
        compiler_params=pltpu.CompilerParams(dimension_semantics=("arbitrary",)),
        name="attention",
    )(table, qor, kvr, lser, xr)

    qbt, rbr, s1 = pl.pallas_call(
        product_kernel,
        out_shape=(
            shape((NZ, HD, TOK), BF16),
            shape((NG, SLOTS, KB, 128), BF16),
            shape((NZ * NX, HD, TOK), BF16),
        ),
        in_specs=[vmem, vmem, hbm, hbm],
        out_specs=(vmem, hbm, vmem),
        scratch_shapes=[
            pltpu.VMEM((NY, TOK, normed_input.shape[1]), BF16),
            pltpu.VMEM((TOK, NZ * HD), BF16),
            pltpu.VMEM((NZ * NX, HD, TOK), F32),
            pltpu.VMEM((NZ * NX, HD, TOK), BF16),
            pltpu.VMEM((NZ * NX, HD, TOK), BF16),
            dma((NZ,)), dma((NZ,)), dma((NG,)), dma((NG,)), dma((NY,)), dma((NY,)), dma((NY + 1,)),
        ],
        compiler_params=pltpu.CompilerParams(collective_id=1, has_side_effects=True),
        name="product",
    )(dqt, rb, normed_input, ag)

    dkv = pl.pallas_call(
        collect_kernel,
        grid=(NZ,),
        out_shape=shape((NZ, TOK, 128), BF16),
        in_specs=[
            smem,
            pl.BlockSpec((1, TOK, 128), lambda i: (i, 0, 0)),
            pl.BlockSpec((NG, SLOTS, KB, 128), lambda i: (0, 0, 0, 0)),
        ],
        out_specs=pl.BlockSpec((1, TOK, 128), lambda i: (i, 0, 0)),
        scratch_shapes=[pltpu.VMEM((TOK, 128), F32)],
        compiler_params=pltpu.CompilerParams(dimension_semantics=("arbitrary",)),
        name="collect",
    )(want, dkvo, rbr)

    dkvr, grad_weight = pl.pallas_call(
        return_kernel,
        out_shape=(shape((NZ, TOK, 128), BF16), shape((HD, TOK), F32)),
        in_specs=[vmem, vmem],
        out_specs=(hbm, vmem),
        scratch_shapes=[pltpu.VMEM((NZ, HD, TOK), BF16)] * 6
        + [dma((NZ,))] * 10
        + [dma((1,))],
        compiler_params=pltpu.CompilerParams(collective_id=2, has_side_effects=True),
        name="return",
    )(dkv, s1)

    width = NZ * HD
    grad_queries, grad_keys, grad_values = pl.pallas_call(
        unpack_kernel,
        grid=(NZ // 2,),
        out_shape=(shape((TOK, width), F32),) * 3,
        in_specs=[
            pl.BlockSpec((2, HD, TOK), lambda i: (i, 0, 0)),
            pl.BlockSpec((2, TOK, 128), lambda i: (i, 0, 0)),
        ],
        out_specs=(pl.BlockSpec((TOK, 128), lambda i: (0, i)),) * 3,
        compiler_params=pltpu.CompilerParams(dimension_semantics=("arbitrary",)),
        name="unpack",
    )(qbt, dkvr)
    return (grad_queries, grad_keys, grad_values, grad_weight)


def solution(mesh):
    return jax.shard_map(
        per_device,
        mesh=mesh,
        in_specs=(
            P("kv", "tp"),
            P("kv", "tp"),
            P("kv", "tp"),
            P("kv", "tp"),
            P("tp", "kv"),
            P("kv", "tp"),
            P("kv", None),
        ),
        out_specs=(P("kv", "tp"), P("kv", "tp"), P("kv", "tp"), P("kv", "tp")),
        check_vma=False,
    )
```
